32 devices in a mesh: kv: 8 (over z, x), tp: 4 (over y, core).
Axes of the slice: x: 2, y: 2, z: 4, core: 2. Of those that a mesh axis runs over, the one named last changes fastest.
Arguments:
- hidden: bfloat16 [512, 4096], P(None, 'kv'), as said below
- norm_gain: bfloat16 [4096], replicated, may hold values from 0.099609375 to 1.8984375
- w_query: bfloat16 [4096, 4096], P('kv', 'tp'), may hold values from -0.09375 to 0.09375
- w_key: bfloat16 [4096, 4096], P('kv', 'tp'), may hold values from -0.09375 to 0.09375
- w_value: bfloat16 [4096, 8192], P('kv', 'tp'), may hold values from -0.09375 to 0.09375
- w_gate: bfloat16 [4096, 8192], P('kv', 'tp'), may hold values from -0.09375 to 0.09375
- w_write: bfloat16 [4096, 32], P('kv', 'tp'), may hold values from -0.09375 to 0.09375
- w_decay: bfloat16 [4096, 32], P('kv', 'tp'), may hold values from -0.09375 to 0.09375
- w_out: bfloat16 [8192, 4096], P('tp', 'kv'), may hold values from -0.0625 to 0.0625
- decay_rate: float32 [32], P('tp'), may hold values from 0 to 4, as said below
- head_gain: float32 [256], replicated, may hold values from 0.1 to 1.9
- carried_state: float32 [128, 32, 128, 256], P('kv', 'tp'), may hold values from -4 to 4
- last_keys: bfloat16 [128, 4, 4096], P('kv', None, 'tp'), may hold values from -6 to 6
- last_values: bfloat16 [128, 4, 8192], P('kv', None, 'tp'), may hold values from -6 to 6
- last_writes: float32 [128, 4, 32], P('kv', None, 'tp'), may hold values from -6 to 6
- last_decays: float32 [128, 4, 32], P('kv', None, 'tp'), may hold values from -6 to 6
- accepted: int32 [128], P('kv'), may hold values from 0 to 4
Outputs:
- mixed_out: bfloat16 [512, 4096], P('tp', 'kv')
- committed: float32 [128, 32, 128, 256], P('kv', 'tp')
The draws below stay inside these ranges and needn't reach their ends.
Inputs may be any that keep to these rules, and one draw needn't show every extreme that they name: `decay_rate`: positive. `hidden`: finite real values.
All inputs are finite; a program needn't handle non-finite values.
Results may differ from the reference program's by a relative error of at most 0.029.
Values may be sent and summed in bfloat16 or wider, within the bound.
A program may use at most 128 MiB of HBM per device.

```python
import math
import jax
import jax.numpy as jnp
from jax import lax

D = 4096
HEADS = 32
DK = 128
DV = 256
PROP = 4
SEQS = 128
TOKENS = 512
N_TP = 4


def draw_hidden(key, part):
    first, second, third = jax.random.split(key, 3)
    group = max(D // 16, 1)
    groups = (D + group - 1) // group
    scales = jnp.exp(jax.random.uniform(first, (groups,), jnp.float32, math.log(0.25), math.log(4.0)))
    channel_scale = scales[jnp.arange(D) // group]
    base = jax.random.normal(second, (TOKENS, D), jnp.float32)
    return (base * channel_scale[None, :]).astype(jnp.bfloat16)


def draw_decay_rate(key, part):
    return jnp.exp(jax.random.uniform(key, (HEADS,), jnp.float32, math.log(0.02), math.log(4.0)))


def with_ends(entries, own_key, smallest, largest):
    dims = entries.shape
    spot = [jax.random.randint(jax.random.fold_in(own_key, axis), (), 0, dims[axis]) for axis in range(len(dims))]
    entries = entries.at[tuple(spot)].set(smallest)
    longest = dims.index(max(dims))
    spot[longest] = (spot[longest] + 1) % dims[longest]
    return entries.at[tuple(spot)].set(largest)


def steps_of(rng, extent, cuts, low, top_value):
    loudness = 1.0
    for axis_at, shards_of in cuts:
        draws = jax.random.uniform(jax.random.fold_in(jax.random.fold_in(rng, 6), axis_at), (shards_of,), jnp.float32, low / len(cuts), top_value / len(cuts))
        loudness = loudness * jnp.repeat(jnp.exp(draws), extent[axis_at] // shards_of).reshape((-1,) + (1,) * (len(extent) - 1 - axis_at))
    return loudness


def gaussian(stream_key, dims, deviation, most, cuts=(), held_as=jnp.bfloat16):
    array = jax.random.normal(stream_key, dims, jnp.float32) * deviation
    if len(cuts) > 0:
        array = steps_of(stream_key, dims, cuts, -0.22, 0.18) * array
    return jnp.clip(array, min=-most, max=most).astype(held_as)


def setup_inputs(seed: int = 0) -> dict:
    streams_of = jax.random.split(jax.random.key(seed), 18)
    return {
        "hidden": draw_hidden(jax.random.fold_in(streams_of[17], 71), 0),
        "norm_gain": jnp.clip(1.0 + 0.18 * jax.random.normal(streams_of[1], (D,), jnp.float32), 0.099609375, 1.8984375).astype(jnp.bfloat16),
        "w_query": gaussian(streams_of[2], (D, HEADS * DK), D ** -0.5, 0.09375, ((0, 8), (1, 4))),
        "w_key": gaussian(streams_of[3], (D, HEADS * DK), D ** -0.5, 0.09375, ((0, 8), (1, 4))),
        "w_value": gaussian(streams_of[4], (D, HEADS * DV), D ** -0.5, 0.09375, ((0, 8), (1, 4))),
        "w_gate": gaussian(streams_of[5], (D, HEADS * DV), D ** -0.5, 0.09375, ((0, 8), (1, 4))),
        "w_write": gaussian(streams_of[6], (D, HEADS), D ** -0.5, 0.09375, ((0, 8), (1, 4))),
        "w_decay": gaussian(streams_of[7], (D, HEADS), D ** -0.5, 0.09375, ((0, 8), (1, 4))),
        "w_out": gaussian(streams_of[8], (HEADS * DV, D), (HEADS * DV) ** -0.5, 0.0625, ((0, 4), (1, 8))),
        "decay_rate": draw_decay_rate(jax.random.fold_in(streams_of[17], 71), 0),
        "head_gain": jnp.clip(1.0 + 0.18 * jax.random.normal(streams_of[10], (DV,), jnp.float32), 0.1, 1.9),
        "carried_state": gaussian(streams_of[11], (SEQS, HEADS, DK, DV), 0.3, 4.0, ((0, 8), (1, 4)), jnp.float32),
        "last_keys": gaussian(streams_of[12], (SEQS, PROP, HEADS * DK), 1.0, 6.0, ((0, 8), (2, 4))),
        "last_values": gaussian(streams_of[13], (SEQS, PROP, HEADS * DV), 1.0, 6.0, ((0, 8), (2, 4))),
        "last_writes": gaussian(streams_of[14], (SEQS, PROP, HEADS), 1.0, 6.0, ((0, 8), (2, 4)), jnp.float32),
        "last_decays": gaussian(streams_of[15], (SEQS, PROP, HEADS), 1.0, 6.0, ((0, 8), (2, 4)), jnp.float32),
        "accepted": with_ends(jax.random.randint(streams_of[16], (SEQS,), 0, PROP + 1), jax.random.fold_in(streams_of[16], 1), 0, PROP).astype(jnp.int32),
    }


norm_eps = 1e-06
highest = lax.Precision.HIGHEST

def unit_rows(matrix):
    return matrix * lax.rsqrt(lax.optimization_barrier(jnp.sum(matrix * matrix, -1, keepdims=True)) + norm_eps)

def corrected(key_rows, values, write_rate, log_decay, start_state):
    proposals = key_rows.shape[2]
    value_width = values.shape[-1]
    running = jnp.cumsum(log_decay, axis=-1)
    causal = jnp.tril(jnp.ones((proposals, proposals), dtype=bool))
    spread = running[..., :, None] - running[..., None, :]
    weights = jnp.where(causal, jnp.exp(jnp.where(causal, spread, 0.0)), 0.0)
    strong_keys = key_rows * write_rate[..., None]
    lower_part = jnp.einsum('bhcd,bhsd->bhcs', strong_keys, key_rows, precision=highest)
    lower_part = lower_part * weights * (1.0 - jnp.eye(proposals, dtype=jnp.float32))
    right_side = jnp.concatenate([values * write_rate[..., None], strong_keys * jnp.exp(running)[..., None]], -1)
    solved_rows = []
    for later in range(proposals):
        current = right_side[..., later, :]
        for early in range(later):
            current = current - lower_part[..., later, early, None] * solved_rows[early]
        solved_rows.append(current)
    solved = jnp.stack(solved_rows, axis=2)
    fresh_values = solved[..., :value_width] - jnp.einsum('bhcd,bhde->bhce', solved[..., value_width:], start_state, precision=highest)
    return (fresh_values, running, weights)

def advance(key_rows, fresh_values, running, start_state):
    tail_decay = jnp.exp(running[..., -1:] - running)
    return start_state * jnp.exp(running[..., -1])[..., None, None] + jnp.einsum('bhcd,bhce->bhde', key_rows * tail_decay[..., None], fresh_values, precision=highest)

def readout(queries, key_rows, fresh_values, running, weights, start_state):
    scores = jnp.einsum('bhcd,bhsd->bhcs', queries, key_rows, precision=highest) * weights
    carried = jnp.einsum('bhcd,bhde->bhce', queries * jnp.exp(running)[..., None], start_state, precision=highest)
    return carried + jnp.einsum('bhcs,bhse->bhce', scores, fresh_values, precision=highest)

def core(proj_query, proj_key, proj_value, proj_gate, proj_write, proj_decay, decay_rate, head_gain, carried_state, last_keys, last_values, last_writes, last_decays, accepted):
    seq_count, head_count, key_width, value_width = carried_state.shape
    proposals = last_keys.shape[1]

    def by_head(matrix, width):
        return jnp.transpose(matrix.reshape(seq_count, proposals, head_count, width), (0, 2, 1, 3))

    def by_head_small(matrix):
        return jnp.transpose(matrix.reshape(seq_count, proposals, head_count), (0, 2, 1))
    rates = decay_rate.astype(jnp.float32)[None, :, None]
    taken = (jnp.arange(proposals, dtype=jnp.int32)[None, :] < accepted[:, None]).astype(jnp.float32)[:, None, :]
    old_keys = unit_rows(by_head(last_keys.astype(jnp.float32), key_width))
    old_values = by_head(last_values.astype(jnp.float32), value_width)
    old_write = jax.nn.sigmoid(by_head_small(last_writes)) * taken
    old_decay = -rates * jax.nn.softplus(by_head_small(last_decays)) * taken
    fresh_values, running, weights = corrected(old_keys, old_values, old_write, old_decay, carried_state)
    committed = advance(old_keys, fresh_values, running, carried_state)
    queries = unit_rows(by_head(jax.nn.silu(proj_query), key_width)) * key_width ** (-0.5)
    key_rows = unit_rows(by_head(jax.nn.silu(proj_key), key_width))
    values = by_head(jax.nn.silu(proj_value), value_width)
    write_rate = jax.nn.sigmoid(by_head_small(proj_write))
    log_decay = -rates * jax.nn.softplus(by_head_small(proj_decay))
    fresh_values, running, weights = corrected(key_rows, values, write_rate, log_decay, committed)
    result = readout(queries, key_rows, fresh_values, running, weights, committed)
    normed = result * lax.rsqrt(lax.optimization_barrier(jnp.mean(result * result, -1, keepdims=True)) + norm_eps) * head_gain.astype(jnp.float32)
    gated = normed * jax.nn.silu(by_head(proj_gate, value_width))
    gated_rows = jnp.transpose(gated, (0, 2, 1, 3)).reshape(seq_count * proposals, head_count * value_width).astype(jnp.bfloat16)
    return (gated_rows, committed)

def reference(hidden, norm_gain, w_query, w_key, w_value, w_gate, w_write, w_decay, w_out, decay_rate, head_gain, carried_state, last_keys, last_values, last_writes, last_decays, accepted):
    wide_rows = hidden.astype(jnp.float32)
    inverse = lax.rsqrt(lax.optimization_barrier(jnp.sum(wide_rows * wide_rows, -1, keepdims=True)) / D + norm_eps)
    scaled = (wide_rows * norm_gain.astype(jnp.float32)).astype(jnp.bfloat16)

    def project(weight):
        return jnp.dot(scaled, weight, preferred_element_type=jnp.float32) * inverse
    gated_rows, committed = core(project(w_query), project(w_key), project(w_value), project(w_gate), project(w_write), project(w_decay), decay_rate, head_gain, carried_state, last_keys, last_values, last_writes, last_decays, accepted)
    grouped = gated_rows.astype(jnp.float32).reshape(TOKENS, N_TP, -1)
    weight_groups = w_out.astype(jnp.float32).reshape(N_TP, -1, D)
    partial_value = jnp.einsum('tmc,mcd->mtd', grouped, weight_groups)
    rounded = lax.optimization_barrier(partial_value.astype(jnp.bfloat16)).astype(jnp.float32)
    mixed_out = lax.optimization_barrier(jnp.sum(rounded, 0)).astype(jnp.bfloat16)
    return (mixed_out, committed)
```

```python
import functools
import jax
import jax.numpy as jnp
from jax import lax
from jax.experimental import pallas as pl
from jax.experimental.pallas import tpu as pltpu
from jax.sharding import PartitionSpec as P

norm_eps = 1e-06
LANES = 128
MESH = pl.DeviceIdType.MESH
VMEM_LIMIT = 60 * 1024 * 1024


def remote(src, dst, send, recv, device):
    return pltpu.make_async_remote_copy(
        src_ref=src, dst_ref=dst, send_sem=send, recv_sem=recv,
        device_id=device, device_id_type=MESH,
    )


def project_kernel(
    nx, nz, plan, width, sq_col, s_ref, small_ref, wq, wk, wv, wg, out_ref, small_out,
    wbuf, own, xs, xr, zs, zr, sm_xr, sm_zs, sm_zr,
    wsem, xss, xrs, zss, zrs, sxs, sxr, szs, szr,
):
    kv, tp = lax.axis_index("kv"), lax.axis_index("tp")
    x, z = lax.rem(kv, nx), lax.div(kv, nx)
    weights = (wq, wk, wv, wg)
    nc = len(plan)
    rows, cw = out_ref.shape[1], out_ref.shape[2]
    x_at = [lax.rem(x + d, nx) for d in range(nx)]
    z_at = [lax.rem(z + d, nz) for d in range(nz)]

    def fetch(c):
        which, off = plan[c]
        return pltpu.make_async_copy(
            weights[which].at[:, pl.ds(off, cw)], wbuf.at[c], wsem.at[c]
        )

    for c in range(nc):
        fetch(c).start()
    barrier = pltpu.get_barrier_semaphore()
    for d in range(1, nx):
        pl.semaphore_signal(barrier, inc=1, device_id=(z * nx + x_at[d], tp), device_id_type=MESH)
    for d in range(1, nz):
        pl.semaphore_signal(barrier, inc=1, device_id=(z_at[d] * nx + x, tp), device_id_type=MESH)
    pl.semaphore_wait(barrier, nx - 1 + nz - 1)

    def small_x(d):
        return remote(small_ref.at[x_at[d]], sm_xr.at[d - 1], sxs.at[d - 1], sxr.at[d - 1],
                      (z * nx + x_at[d], tp))

    def small_z(d):
        return remote(sm_zs.at[z_at[d]], sm_zr.at[d - 1], szs.at[d - 1], szr.at[d - 1],
                      (z_at[d] * nx + x, tp))

    def big_x(c, d):
        return remote(xs.at[c, d - 1], xr.at[c, d - 1], xss.at[c, d - 1], xrs.at[c, d - 1],
                      (z * nx + x_at[d], tp))

    def big_z(c, d):
        return remote(zs.at[c, z_at[d]], zr.at[c, d - 1], zss.at[c, d - 1], zrs.at[c, d - 1],
                      (z_at[d] * nx + x, tp))

    z_order = sorted(range(1, nz), key=lambda d: -min(d, nz - d))
    for d in range(1, nx):
        small_x(d).start()

    def multiply(c, carry):
        pltpu.make_async_copy(wbuf.at[c], wbuf.at[c], wsem.at[c]).wait()
        for d in range(1, nx):
            part = jnp.dot(s_ref[x_at[d]], wbuf[c], preferred_element_type=jnp.float32)
            xs[c, d - 1] = part.astype(jnp.bfloat16).reshape(nz, rows, cw)
            big_x(c, d).start()
        own[c] = jnp.dot(
            s_ref[x], wbuf[c], preferred_element_type=jnp.float32
        ).reshape(nz, rows, cw)
        return carry

    lax.fori_loop(0, nc, multiply, 0)

    total = small_ref[x].astype(jnp.float32)
    for d in range(1, nx):
        small_x(d).wait()
        total = total + sm_xr[d - 1].astype(jnp.float32)
    sm_zs[...] = total.astype(jnp.bfloat16)
    for d in z_order:
        small_z(d).start()

    def middle(c, carry):
        summed = own[c]
        for d in range(1, nx):
            big_x(c, d).wait()
            summed = summed + xr[c, d - 1].astype(jnp.float32)
        own[c] = summed
        zs[c] = summed.astype(jnp.bfloat16)
        for d in z_order:
            big_z(c, d).start()
        return carry

    lax.fori_loop(0, nc, middle, 0)

    small = sm_zs[z].astype(jnp.float32)
    for d in range(1, nz):
        small_z(d).wait()
        small = small + sm_zr[d - 1].astype(jnp.float32)
    inverse = lax.rsqrt(small[:, sq_col:sq_col + 1] / width + norm_eps)
    small_out[...] = small * inverse

    def finish(c, carry):
        summed = own[c, z]
        for d in range(1, nz):
            big_z(c, d).wait()
            summed = summed + zr[c, d - 1].astype(jnp.float32)
        out_ref[c] = summed * inverse
        return carry

    lax.fori_loop(0, nc, finish, 0)


def project(nx, nz, scaled, small, weights, sq_col, width):
    depth = scaled.shape[1]
    rows = scaled.shape[0] // (nx * nz)
    cw = min(512, weights[0].shape[1])
    plan = [(i, off) for i, w in enumerate(weights) for off in range(0, w.shape[1], cw)]
    nc = len(plan)
    by_x = jnp.transpose(scaled.reshape(nz, nx, rows, depth), (1, 0, 2, 3))
    by_x = by_x.reshape(nx, nz * rows, depth)
    small_x = jnp.transpose(small.reshape(nz, nx, rows, LANES), (1, 0, 2, 3))
    bf, f32, dma = jnp.bfloat16, jnp.float32, pltpu.SemaphoreType.DMA
    px, pz = max(nx - 1, 1), max(nz - 1, 1)
    vmem = pl.BlockSpec(memory_space=pltpu.VMEM)
    hbm = pl.BlockSpec(memory_space=pl.ANY)
    return plan, pl.pallas_call(
        functools.partial(project_kernel, nx, nz, plan, width, sq_col),
        out_shape=(
            jax.ShapeDtypeStruct((nc, rows, cw), f32),
            jax.ShapeDtypeStruct((rows, LANES), f32),
        ),
        in_specs=[vmem, vmem, hbm, hbm, hbm, hbm],
        out_specs=(vmem, vmem),
        scratch_shapes=[
            pltpu.VMEM((nc, depth, cw), bf),
            pltpu.VMEM((nc, nz, rows, cw), f32),
            pltpu.VMEM((nc, px, nz, rows, cw), bf),
            pltpu.VMEM((nc, px, nz, rows, cw), bf),
            pltpu.VMEM((nc, nz, rows, cw), bf),
            pltpu.VMEM((nc, pz, rows, cw), bf),
            pltpu.VMEM((px, nz, rows, LANES), bf),
            pltpu.VMEM((nz, rows, LANES), bf),
            pltpu.VMEM((pz, rows, LANES), bf),
            dma((nc,)),
            dma((nc, px)), dma((nc, px)), dma((nc, pz)), dma((nc, pz)),
            dma((px,)), dma((px,)), dma((pz,)), dma((pz,)),
        ],
        compiler_params=pltpu.CompilerParams(
            collective_id=0, has_side_effects=True, vmem_limit_bytes=VMEM_LIMIT
        ),
    )(by_x, small_x, *weights)


def silu(v):
    return v * jax.nn.sigmoid(v)


def unit(v):
    return v * lax.rsqrt(jnp.sum(v * v, -1, keepdims=True) + norm_eps)


def solve(keys, values, write, decay):
    steps = len(keys)
    running = [decay[0]]
    for t in range(1, steps):
        running.append(running[-1] + decay[t])
    strong = [keys[t] * write[t] for t in range(steps)]
    u_val, u_key = [], []
    for t in range(steps):
        cur_v = values[t] * write[t]
        cur_k = strong[t] * jnp.exp(running[t])
        for s in range(t):
            low = jnp.sum(strong[t] * keys[s], -1, keepdims=True)
            low = low * jnp.exp(running[t] - running[s])
            cur_v = cur_v - low * u_val[s]
            cur_k = cur_k - low * u_key[s]
        u_val.append(cur_v)
        u_key.append(cur_k)
    return running, u_val, u_key


def core_kernel(
    heads, q_ref, k_ref, v_ref, g_ref, small_ref, lk_ref, lv_ref, lsmall_ref, rate_ref,
    gain_ref, state_ref, gated_ref, com_ref, left, prod, kd, fr, dec, wide_k, wide_v, gout,
):
    h = pl.program_id(0)
    seqs = state_ref.shape[0]
    steps = q_ref.shape[1] // seqs
    dk, dv = q_ref.shape[2], v_ref.shape[2]
    pad = left.shape[1]
    bf, f32 = jnp.bfloat16, jnp.float32

    def at_t(ref, t):
        return ref[pl.ds(t, seqs, stride=steps), :]

    tiles = dv // LANES

    def value_at(ref, t):
        return jnp.concatenate([at_t(ref.at[j], t) for j in range(tiles)], -1)

    def cut(j):
        return slice(j * LANES, (j + 1) * LANES)

    lane = lax.broadcasted_iota(jnp.int32, (seqs, LANES), 1)

    def column(mat, col):
        return jnp.sum(jnp.where(lane == col, mat, 0.0), -1, keepdims=True)

    rate = column(jnp.broadcast_to(rate_ref[...], (seqs, LANES)), h)
    every = range(steps)

    wide_k[...] = lk_ref[...].astype(f32)
    for j in range(tiles):
        wide_v[j] = lv_ref[:, cut(j)].astype(f32)
    old = [at_t(lsmall_ref, t) for t in every]
    taken = [column(m, 2 * heads) for m in old]
    write = [jax.nn.sigmoid(column(old[t], h)) * taken[t] for t in every]
    decay = [-rate * jax.nn.softplus(column(old[t], heads + h)) * taken[t] for t in every]
    keys = [unit(at_t(wide_k, t)) for t in every]
    running, u_val, u_key = solve(keys, [value_at(wide_v, t) for t in every], write, decay)
    for t in every:
        left[:, t, :] = u_key[t]
        kd[:, t, :] = keys[t] * jnp.exp(running[-1] - running[t])
    dec[...] = jnp.broadcast_to(jnp.exp(running[-1]), (seqs, dv))
    for t in range(steps, pad):
        left[:, t, :] = jnp.zeros((seqs, dk), f32)
        kd[:, t, :] = jnp.zeros((seqs, dk), f32)
        fr[:, t, :] = jnp.zeros((seqs, dv), f32)
    for b in range(seqs):
        prod[b] = jnp.dot(
            left[b].astype(bf), state_ref[b, 0].astype(bf), preferred_element_type=f32
        )
    for t in every:
        fr[:, t, :] = u_val[t] - prod[:, t, :]

    small = [at_t(small_ref, t) for t in every]
    write = [jax.nn.sigmoid(column(small[t], h)) for t in every]
    decay = [-rate * jax.nn.softplus(column(small[t], heads + h)) for t in every]
    queries = [unit(silu(at_t(q_ref.at[0], t))) * dk ** (-0.5) for t in every]
    for j in range(tiles):
        wide_v[j] = silu(v_ref[0, :, cut(j)])
    keys = [unit(silu(at_t(k_ref.at[0], t))) for t in every]
    running, u_val, u_key = solve(keys, [value_at(wide_v, t) for t in every], write, decay)
    for t in every:
        left[:, t, :] = u_key[t]
        left[:, steps + t, :] = queries[t] * jnp.exp(running[t])
    for b in range(seqs):
        added = lax.dot_general(
            kd[b].astype(bf), fr[b].astype(bf), (((0,), (0,)), ((), ())),
            preferred_element_type=f32,
        )
        after = state_ref[b, 0] * dec[b:b + 1, :] + added
        com_ref[b, 0] = after
        prod[b] = jnp.dot(left[b].astype(bf), after.astype(bf), preferred_element_type=f32)

    gain = gain_ref[...]
    fresh = [u_val[t] - prod[:, t, :] for t in every]
    for t in every:
        result = prod[:, steps + t, :]
        for s in range(t + 1):
            score = jnp.sum(queries[t] * keys[s], -1, keepdims=True)
            score = score * jnp.exp(running[t] - running[s])
            result = result + score * fresh[s]
        scale = lax.rsqrt(jnp.mean(result * result, -1, keepdims=True) + norm_eps)
        normed = result * scale * gain
        for j in range(tiles):
            gout[j, pl.ds(t, seqs, stride=steps), :] = normed[:, cut(j)]
    for j in range(tiles):
        gated_ref[:, cut(j)] = (gout[j] * silu(g_ref[0, :, cut(j)])).astype(bf)


def core(plan, projected, small, last_keys, last_values, last_small, rates, head_gain, state):
    seqs, heads, dk, dv = state.shape
    steps = last_keys.shape[1]
    rows = seqs * steps
    cw = projected.shape[2]
    kpc, vpc = cw // dk, cw // dv
    first = [next(c for c, (w, _) in enumerate(plan) if w == i) for i in range(4)]
    pad = 2 * steps
    f32 = jnp.float32

    def key_block(base):
        return pl.BlockSpec((1, rows, dk), lambda h: (base + h // kpc, 0, h % kpc))

    def val_block(base):
        return pl.BlockSpec((1, rows, dv), lambda h: (base + h // vpc, 0, h % vpc))

    def whole(shape):
        return pl.BlockSpec(shape, lambda h: (0,) * len(shape))

    state_block = pl.BlockSpec((seqs, 1, dk, dv), lambda h: (0, h, 0, 0))
    return pl.pallas_call(
        functools.partial(core_kernel, heads),
        grid=(heads,),
        out_shape=(
            jax.ShapeDtypeStruct((rows, heads * dv), jnp.bfloat16),
            jax.ShapeDtypeStruct(state.shape, f32),
        ),
        in_specs=[
            key_block(first[0]), key_block(first[1]), val_block(first[2]), val_block(first[3]),
            whole((rows, LANES)),
            pl.BlockSpec((rows, dk), lambda h: (0, h)),
            pl.BlockSpec((rows, dv), lambda h: (0, h)),
            whole((rows, LANES)), whole((1, LANES)), whole((1, dv)), state_block,
        ],
        out_specs=(pl.BlockSpec((rows, dv), lambda h: (0, h)), state_block),
        scratch_shapes=[
            pltpu.VMEM((seqs, pad, dk), f32),
            pltpu.VMEM((seqs, pad, dv), f32),
            pltpu.VMEM((seqs, pad, dk), f32),
            pltpu.VMEM((seqs, pad, dv), f32),
            pltpu.VMEM((seqs, dv), f32),
            pltpu.VMEM((rows, dk), f32),
            pltpu.VMEM((dv // LANES, rows, LANES), f32),
            pltpu.VMEM((dv // LANES, rows, LANES), f32),
        ],
        compiler_params=pltpu.CompilerParams(vmem_limit_bytes=VMEM_LIMIT),
    )(
        projected, projected, projected, projected, small,
        last_keys.reshape(rows, heads * dk), last_values.reshape(rows, heads * dv),
        last_small, rates, head_gain, state,
    )


def output_kernel(
    nx, nz, ntp, g_ref, w_ref, out_ref, held, parts, got,
    zss, zrs, xss, xrs, tss, trs, csem,
):
    kv, tp = lax.axis_index("kv"), lax.axis_index("tp")
    x, z = lax.rem(kv, nx), lax.div(kv, nx)
    rows = g_ref.shape[0]
    per = out_ref.shape[0]
    pieces = nx * rows // per
    x_at = [lax.rem(x + d, nx) for d in range(nx)]
    z_at = [lax.rem(z + d, nz) for d in range(nz)]
    z_from = [lax.rem(z + nz - d, nz) for d in range(nz)]
    x_from = [lax.rem(x + nx - d, nx) for d in range(nx)]
    t_at = [lax.rem(tp + d, ntp) for d in range(ntp)]

    barrier = pltpu.get_barrier_semaphore()
    for d in range(1, nx):
        pl.semaphore_signal(barrier, inc=1, device_id=(z * nx + x_at[d], tp), device_id_type=MESH)
    for d in range(1, nz):
        pl.semaphore_signal(barrier, inc=1, device_id=(z_at[d] * nx + x, tp), device_id_type=MESH)
    for d in range(1, ntp):
        pl.semaphore_signal(barrier, inc=1, device_id=(kv, t_at[d]), device_id_type=MESH)
    local = pltpu.make_async_copy(g_ref, held.at[z, x], csem)
    local.start()
    pl.semaphore_wait(barrier, nx - 1 + nz - 1 + ntp - 1)

    def along_z(d):
        return remote(g_ref, held.at[z, x], zss.at[d], zrs.at[d], (z_at[d] * nx + x, tp))

    def landed_z(k):
        return remote(g_ref, held.at[z_from[k], x], zss.at[k], zrs.at[k],
                      (z_at[k] * nx + x, tp))

    def along_x(k, d):
        return remote(held.at[z_from[k], x], held.at[z_from[k], x],
                      xss.at[k, d], xrs.at[k, d], (z * nx + x_at[d], tp))

    def landed_x(k, d):
        return remote(held.at[z_from[k], x], held.at[z_from[k], x_from[d]],
                      xss.at[k, d], xrs.at[k, d], (z * nx + x_at[d], tp))

    def own_x(d):
        return remote(g_ref, held.at[z, x], xss.at[0, d], xrs.at[0, d],
                      (z * nx + x_at[d], tp))

    for d in range(1, nz):
        along_z(d).start()
    for d in range(1, nx):
        own_x(d).start()
    local.wait()
    for k in range(nz):
        if k > 0:
            landed_z(k).wait_recv()
            for d in range(1, nx):
                along_x(k, d).start()

    def to_tp(block, j):
        target = block * pieces + j
        return target

    for k in range(nz):
        for d in range(1, nx):
            landed_x(k, d).wait_recv()
        block = z_from[k]
        product = jnp.dot(
            held[block].reshape(nx * rows, held.shape[3]), w_ref[...],
            preferred_element_type=jnp.float32,
        )
        for j in range(pieces):
            parts[block * pieces + j] = product[j * per:(j + 1) * per].astype(jnp.bfloat16)
            target = block * pieces + j

            @pl.when(target != tp)
            def _():
                remote(parts.at[target], got.at[tp], tss.at[target], trs.at[tp],
                       (kv, target)).start()

    summed = parts[tp].astype(jnp.float32)
    for d in range(1, ntp):
        source = t_at[d]
        remote(parts.at[source], got.at[source], tss.at[source], trs.at[source],
               (kv, source)).wait()
        summed = summed + got[source].astype(jnp.float32)
    out_ref[...] = summed.astype(out_ref.dtype)
    for d in range(1, nz):
        along_z(d).wait_send()
    for d in range(1, nx):
        own_x(d).wait_send()
        for k in range(1, nz):
            along_x(k, d).wait_send()


def output(nx, nz, ntp, gated, w_out):
    rows, depth = gated.shape
    columns = w_out.shape[1]
    per = rows * nx * nz // ntp
    bf, dma = jnp.bfloat16, pltpu.SemaphoreType.DMA
    vmem = pl.BlockSpec(memory_space=pltpu.VMEM)
    return pl.pallas_call(
        functools.partial(output_kernel, nx, nz, ntp),
        out_shape=jax.ShapeDtypeStruct((per, columns), bf),
        in_specs=[vmem, vmem],
        out_specs=vmem,
        scratch_shapes=[
            pltpu.VMEM((nz, nx, rows, depth), bf),
            pltpu.VMEM((ntp, per, columns), bf),
            pltpu.VMEM((ntp, per, columns), bf),
            dma((nz,)), dma((nz,)), dma((nz, nx)), dma((nz, nx)),
            dma((ntp,)), dma((ntp,)), dma(()),
        ],
        compiler_params=pltpu.CompilerParams(
            collective_id=1, has_side_effects=True, vmem_limit_bytes=VMEM_LIMIT
        ),
    )(gated, w_out)


def per_device(
    nkv, ntp, hidden, norm_gain, w_query, w_key, w_value, w_gate, w_write, w_decay, w_out,
    decay_rate, head_gain, carried_state, last_keys, last_values, last_writes, last_decays,
    accepted,
):
    f32 = jnp.float32
    nz = 4 if nkv % 4 == 0 else 1
    nx = nkv // nz
    local_width = hidden.shape[1]
    seqs, heads = carried_state.shape[:2]
    steps = last_keys.shape[1]
    rows = seqs * steps
    wide = hidden.astype(f32)
    local_sq = jnp.sum(wide * wide, -1, keepdims=True)
    gain = lax.dynamic_slice_in_dim(norm_gain, lax.axis_index("kv") * local_width, local_width)
    scaled = (wide * gain.astype(f32)).astype(jnp.bfloat16)
    w_small = jnp.concatenate([w_write, w_decay], 1)
    small = jnp.dot(scaled, w_small, preferred_element_type=f32)
    fill = LANES - 2 * heads - 1
    small = jnp.concatenate(
        [small, local_sq, jnp.zeros((small.shape[0], fill), f32)], 1
    ).astype(jnp.bfloat16)
    plan, (projected, small) = project(
        nx, nz, scaled, small, (w_query, w_key, w_value, w_gate), 2 * heads, local_width * nkv
    )
    taken = (jnp.arange(steps, dtype=jnp.int32)[None, :] < accepted[:, None]).astype(f32)
    last_small = jnp.concatenate(
        [last_writes.reshape(rows, heads), last_decays.reshape(rows, heads),
         taken.reshape(rows, 1), jnp.zeros((rows, fill), f32)], 1
    )
    rates = jnp.pad(decay_rate, (0, LANES - heads))[None, :]
    gated, committed = core(
        plan, projected, small, last_keys, last_values, last_small, rates,
        head_gain[None, :], carried_state,
    )
    return (output(nx, nz, ntp, gated, w_out), committed)


def solution(mesh):
    return jax.shard_map(
        functools.partial(per_device, mesh.shape["kv"], mesh.shape["tp"]),
        mesh=mesh,
        in_specs=(
            P(None, "kv"),
            P(),
            P("kv", "tp"),
            P("kv", "tp"),
            P("kv", "tp"),
            P("kv", "tp"),
            P("kv", "tp"),
            P("kv", "tp"),
            P("tp", "kv"),
            P("tp"),
            P(),
            P("kv", "tp", None, None),
            P("kv", None, "tp"),
            P("kv", None, "tp"),
            P("kv", None, "tp"),
            P("kv", None, "tp"),
            P("kv"),
        ),
        out_specs=(P("tp", "kv"), P("kv", "tp", None, None)),
        check_vma=False,
    )
```

```python
import functools
import jax
import jax.numpy as jnp
from jax import lax
from jax.experimental import pallas as pl
from jax.experimental.pallas import tpu as pltpu
from jax.sharding import PartitionSpec as P

norm_eps = 1e-06
LANES = 128
MESH = pl.DeviceIdType.MESH
VMEM_LIMIT = 60 * 1024 * 1024


def remote(src, dst, send, recv, device):
    return pltpu.make_async_remote_copy(
        src_ref=src, dst_ref=dst, send_sem=send, recv_sem=recv,
        device_id=device, device_id_type=MESH,
    )


def project_kernel(
    nx, nz, plan, width, sq_col, h_ref, n_ref, ws_ref, wq, wk, wv, wg, out_ref, small_out,
    s_ref, small_ref, wbuf, own, xs, xr, zs, zr, sm_xr, sm_zs, sm_zr,
    wsem, xss, xrs, zss, zrs, sxs, sxr, szs, szr,
):
    kv, tp = lax.axis_index("kv"), lax.axis_index("tp")
    x, z = lax.rem(kv, nx), lax.div(kv, nx)
    weights = (wq, wk, wv, wg)
    nc = len(plan)
    rows, cw = out_ref.shape[1], out_ref.shape[2]
    x_at = [lax.rem(x + d, nx) for d in range(nx)]
    z_at = [lax.rem(z + d, nz) for d in range(nz)]

    def fetch(c):
        which, off = plan[c]
        return pltpu.make_async_copy(
            weights[which].at[:, pl.ds(off, cw)], wbuf.at[c], wsem.at[c]
        )

    for c in range(nc):
        fetch(c).start()
    barrier = pltpu.get_barrier_semaphore()
    for d in range(1, nx):
        pl.semaphore_signal(barrier, inc=1, device_id=(z * nx + x_at[d], tp), device_id_type=MESH)
    for d in range(1, nz):
        pl.semaphore_signal(barrier, inc=1, device_id=(z_at[d] * nx + x, tp), device_id_type=MESH)
    gain = n_ref[...].astype(jnp.float32)
    lane = lax.broadcasted_iota(jnp.int32, (rows, LANES), 1)
    for i in range(nx):
        for j in range(nz):
            wide = h_ref[(j * nx + i) * rows:(j * nx + i + 1) * rows].astype(jnp.float32)
            scaled = (wide * gain).astype(jnp.bfloat16)
            s_ref[i, j * rows:(j + 1) * rows] = scaled
            part = jnp.dot(scaled, ws_ref[...], preferred_element_type=jnp.float32)
            square = jnp.sum(wide * wide, -1, keepdims=True)
            small_ref[i, j] = jnp.where(lane == sq_col, square, part).astype(jnp.bfloat16)
    pl.semaphore_wait(barrier, nx - 1 + nz - 1)

    def small_x(d):
        return remote(small_ref.at[x_at[d]], sm_xr.at[d - 1], sxs.at[d - 1], sxr.at[d - 1],
                      (z * nx + x_at[d], tp))

    def small_z(d):
        return remote(sm_zs.at[z_at[d]], sm_zr.at[d - 1], szs.at[d - 1], szr.at[d - 1],
                      (z_at[d] * nx + x, tp))

    def big_x(c, d):
        return remote(xs.at[c, d - 1], xr.at[c, d - 1], xss.at[c, d - 1], xrs.at[c, d - 1],
                      (z * nx + x_at[d], tp))

    def big_z(c, d):
        return remote(zs.at[c, z_at[d]], zr.at[c, d - 1], zss.at[c, d - 1], zrs.at[c, d - 1],
                      (z_at[d] * nx + x, tp))

    z_order = sorted(range(1, nz), key=lambda d: -min(d, nz - d))
    for d in range(1, nx):
        small_x(d).start()

    def multiply(c, carry):
        pltpu.make_async_copy(wbuf.at[c], wbuf.at[c], wsem.at[c]).wait()
        for d in range(1, nx):
            part = jnp.dot(s_ref[x_at[d]], wbuf[c], preferred_element_type=jnp.float32)
            xs[c, d - 1] = part.astype(jnp.bfloat16).reshape(nz, rows, cw)
            big_x(c, d).start()
        own[c] = jnp.dot(
            s_ref[x], wbuf[c], preferred_element_type=jnp.float32
        ).reshape(nz, rows, cw)
        return carry

    lax.fori_loop(0, nc, multiply, 0)

    total = small_ref[x].astype(jnp.float32)
    for d in range(1, nx):
        small_x(d).wait()
        total = total + sm_xr[d - 1].astype(jnp.float32)
    sm_zs[...] = total.astype(jnp.bfloat16)
    for d in z_order:
        small_z(d).start()

    def middle(c, carry):
        summed = own[c]
        for d in range(1, nx):
            big_x(c, d).wait()
            summed = summed + xr[c, d - 1].astype(jnp.float32)
        own[c] = summed
        zs[c] = summed.astype(jnp.bfloat16)
        for d in z_order:
            big_z(c, d).start()
        return carry

    lax.fori_loop(0, nc, middle, 0)

    small = sm_zs[z].astype(jnp.float32)
    for d in range(1, nz):
        small_z(d).wait()
        small = small + sm_zr[d - 1].astype(jnp.float32)
    inverse = lax.rsqrt(small[:, sq_col:sq_col + 1] / width + norm_eps)
    small_out[...] = small * inverse

    def finish(c, carry):
        summed = own[c, z]
        for d in range(1, nz):
            big_z(c, d).wait()
            summed = summed + zr[c, d - 1].astype(jnp.float32)
        out_ref[c] = summed * inverse
        return carry

    lax.fori_loop(0, nc, finish, 0)


def project(nx, nz, hidden, gain, w_small, weights, sq_col, width):
    depth = hidden.shape[1]
    rows = hidden.shape[0] // (nx * nz)
    cw = min(512, weights[0].shape[1])
    plan = [(i, off) for i, w in enumerate(weights) for off in range(0, w.shape[1], cw)]
    nc = len(plan)
    bf, f32, dma = jnp.bfloat16, jnp.float32, pltpu.SemaphoreType.DMA
    px, pz = max(nx - 1, 1), max(nz - 1, 1)
    vmem = pl.BlockSpec(memory_space=pltpu.VMEM)
    hbm = pl.BlockSpec(memory_space=pl.ANY)
    return plan, pl.pallas_call(
        functools.partial(project_kernel, nx, nz, plan, width, sq_col),
        out_shape=(
            jax.ShapeDtypeStruct((nc, rows, cw), f32),
            jax.ShapeDtypeStruct((rows, LANES), f32),
        ),
        in_specs=[vmem, vmem, vmem, hbm, hbm, hbm, hbm],
        out_specs=(vmem, vmem),
        scratch_shapes=[
            pltpu.VMEM((nx, nz * rows, depth), bf),
            pltpu.VMEM((nx, nz, rows, LANES), bf),
            pltpu.VMEM((nc, depth, cw), bf),
            pltpu.VMEM((nc, nz, rows, cw), f32),
            pltpu.VMEM((nc, px, nz, rows, cw), bf),
            pltpu.VMEM((nc, px, nz, rows, cw), bf),
            pltpu.VMEM((nc, nz, rows, cw), bf),
            pltpu.VMEM((nc, pz, rows, cw), bf),
            pltpu.VMEM((px, nz, rows, LANES), bf),
            pltpu.VMEM((nz, rows, LANES), bf),
            pltpu.VMEM((pz, rows, LANES), bf),
            dma((nc,)),
            dma((nc, px)), dma((nc, px)), dma((nc, pz)), dma((nc, pz)),
            dma((px,)), dma((px,)), dma((pz,)), dma((pz,)),
        ],
        compiler_params=pltpu.CompilerParams(
            collective_id=0, has_side_effects=True, vmem_limit_bytes=VMEM_LIMIT
        ),
    )(hidden, gain, w_small, *weights)


def silu(v):
    return v * jax.nn.sigmoid(v)


def unit(v):
    return v * lax.rsqrt(jnp.sum(v * v, -1, keepdims=True) + norm_eps)


def solve(keys, values, write, decay):
    steps = len(keys)
    running = [decay[0]]
    for t in range(1, steps):
        running.append(running[-1] + decay[t])
    strong = [keys[t] * write[t] for t in range(steps)]
    u_val, u_key = [], []
    for t in range(steps):
        cur_v = values[t] * write[t]
        cur_k = strong[t] * jnp.exp(running[t])
        for s in range(t):
            low = jnp.sum(strong[t] * keys[s], -1, keepdims=True)
            low = low * jnp.exp(running[t] - running[s])
            cur_v = cur_v - low * u_val[s]
            cur_k = cur_k - low * u_key[s]
        u_val.append(cur_v)
        u_key.append(cur_k)
    return running, u_val, u_key


def core_kernel(
    heads, q_ref, k_ref, v_ref, g_ref, small_ref, lk_ref, lv_ref, lw_ref, ld_ref, acc_ref, rate_ref,
    gain_ref, state_ref, gated_ref, com_ref, left, prod, kd, fr, dec, old_k, old_v, wide_v, gout,
):
    h = pl.program_id(0)
    seqs = state_ref.shape[0]
    steps = q_ref.shape[1] // seqs
    dk, dv = q_ref.shape[2], v_ref.shape[2]
    pad = left.shape[1]
    bf, f32 = jnp.bfloat16, jnp.float32

    def at_t(ref, t):
        return ref[pl.ds(t, seqs, stride=steps), :]

    tiles = dv // LANES

    def value_at(ref, t):
        return jnp.concatenate([at_t(ref.at[j], t) for j in range(tiles)], -1)

    def cut(j):
        return slice(j * LANES, (j + 1) * LANES)

    lane = lax.broadcasted_iota(jnp.int32, (seqs, LANES), 1)

    few = lax.broadcasted_iota(jnp.int32, (seqs, heads), 1)

    def column(mat, col):
        index = lane if mat.shape[1] == LANES else few
        return jnp.sum(jnp.where(index == col, mat, 0.0), -1, keepdims=True)

    rate = column(jnp.broadcast_to(rate_ref[...], (seqs, heads)), h)
    every = range(steps)

    old_k[...] = lk_ref[...].astype(f32)
    old_v[...] = lv_ref[...].astype(f32)
    taken = [(acc_ref[...] > t).astype(f32) for t in every]
    write = [jax.nn.sigmoid(column(lw_ref[:, t, :], h)) * taken[t] for t in every]
    decay = [-rate * jax.nn.softplus(column(ld_ref[:, t, :], h)) * taken[t] for t in every]
    keys = [unit(old_k[:, t, :]) for t in every]
    running, u_val, u_key = solve(keys, [old_v[:, t, :] for t in every], write, decay)
    for t in every:
        left[:, t, :] = u_key[t]
        kd[:, t, :] = keys[t] * jnp.exp(running[-1] - running[t])
    dec[...] = jnp.broadcast_to(jnp.exp(running[-1]), (seqs, dv))
    for t in range(steps, pad):
        left[:, t, :] = jnp.zeros((seqs, dk), f32)
        kd[:, t, :] = jnp.zeros((seqs, dk), f32)
        fr[:, t, :] = jnp.zeros((seqs, dv), f32)
    for b in range(seqs):
        prod[b] = jnp.dot(
            left[b].astype(bf), state_ref[b, 0].astype(bf), preferred_element_type=f32
        )
    for t in every:
        fr[:, t, :] = u_val[t] - prod[:, t, :]

    small = [at_t(small_ref, t) for t in every]
    write = [jax.nn.sigmoid(column(small[t], h)) for t in every]
    decay = [-rate * jax.nn.softplus(column(small[t], heads + h)) for t in every]
    queries = [unit(silu(at_t(q_ref.at[0], t))) * dk ** (-0.5) for t in every]
    for j in range(tiles):
        wide_v[j] = silu(v_ref[0, :, cut(j)])
    keys = [unit(silu(at_t(k_ref.at[0], t))) for t in every]
    running, u_val, u_key = solve(keys, [value_at(wide_v, t) for t in every], write, decay)
    for t in every:
        left[:, t, :] = u_key[t]
        left[:, steps + t, :] = queries[t] * jnp.exp(running[t])
    for b in range(seqs):
        added = lax.dot_general(
            kd[b].astype(bf), fr[b].astype(bf), (((0,), (0,)), ((), ())),
            preferred_element_type=f32,
        )
        after = state_ref[b, 0] * dec[b:b + 1, :] + added
        com_ref[b, 0] = after
        prod[b] = jnp.dot(left[b].astype(bf), after.astype(bf), preferred_element_type=f32)

    gain = gain_ref[...]
    fresh = [u_val[t] - prod[:, t, :] for t in every]
    for t in every:
        result = prod[:, steps + t, :]
        for s in range(t + 1):
            score = jnp.sum(queries[t] * keys[s], -1, keepdims=True)
            score = score * jnp.exp(running[t] - running[s])
            result = result + score * fresh[s]
        scale = lax.rsqrt(jnp.mean(result * result, -1, keepdims=True) + norm_eps)
        normed = result * scale * gain
        for j in range(tiles):
            gout[j, pl.ds(t, seqs, stride=steps), :] = normed[:, cut(j)]
    for j in range(tiles):
        gated_ref[:, cut(j)] = (gout[j] * silu(g_ref[0, :, cut(j)])).astype(bf)


def core(plan, projected, small, last_keys, last_values, last_writes, last_decays, accepted,
         rates, head_gain, state):
    seqs, heads, dk, dv = state.shape
    steps = last_keys.shape[1]
    rows = seqs * steps
    cw = projected.shape[2]
    kpc, vpc = cw // dk, cw // dv
    first = [next(c for c, (w, _) in enumerate(plan) if w == i) for i in range(4)]
    pad = 2 * steps
    f32 = jnp.float32

    def key_block(base):
        return pl.BlockSpec((1, rows, dk), lambda h: (base + h // kpc, 0, h % kpc))

    def val_block(base):
        return pl.BlockSpec((1, rows, dv), lambda h: (base + h // vpc, 0, h % vpc))

    def whole(shape):
        return pl.BlockSpec(shape, lambda h: (0,) * len(shape))

    state_block = pl.BlockSpec((seqs, 1, dk, dv), lambda h: (0, h, 0, 0))
    return pl.pallas_call(
        functools.partial(core_kernel, heads),
        grid=(heads,),
        out_shape=(
            jax.ShapeDtypeStruct((rows, heads * dv), jnp.bfloat16),
            jax.ShapeDtypeStruct(state.shape, f32),
        ),
        in_specs=[
            key_block(first[0]), key_block(first[1]), val_block(first[2]), val_block(first[3]),
            whole((rows, LANES)),
            pl.BlockSpec((seqs, steps, dk), lambda h: (0, 0, h)),
            pl.BlockSpec((seqs, steps, dv), lambda h: (0, 0, h)),
            whole((seqs, steps, heads)), whole((seqs, steps, heads)), whole((seqs, 1)),
            whole((1, heads)), whole((1, dv)), state_block,
        ],
        out_specs=(pl.BlockSpec((rows, dv), lambda h: (0, h)), state_block),
        scratch_shapes=[
            pltpu.VMEM((seqs, pad, dk), f32),
            pltpu.VMEM((seqs, pad, dv), f32),
            pltpu.VMEM((seqs, pad, dk), f32),
            pltpu.VMEM((seqs, pad, dv), f32),
            pltpu.VMEM((seqs, dv), f32),
            pltpu.VMEM((seqs, steps, dk), f32),
            pltpu.VMEM((seqs, steps, dv), f32),
            pltpu.VMEM((dv // LANES, rows, LANES), f32),
            pltpu.VMEM((dv // LANES, rows, LANES), f32),
        ],
        compiler_params=pltpu.CompilerParams(vmem_limit_bytes=VMEM_LIMIT),
    )(
        projected, projected, projected, projected, small,
        last_keys, last_values, last_writes, last_decays, accepted, rates, head_gain, state,
    )


def output_kernel(
    nx, nz, ntp, g_ref, w_hbm, out_ref, held, parts, got, w_ref,
    zss, zrs, xss, xrs, tss, trs, csem, wsem,
):
    kv, tp = lax.axis_index("kv"), lax.axis_index("tp")
    x, z = lax.rem(kv, nx), lax.div(kv, nx)
    halves, rows, depth = held.shape[2:]
    per = out_ref.shape[0]
    pieces = nx * rows // per
    x_at = [lax.rem(x + d, nx) for d in range(nx)]
    t_at = [lax.rem(tp + d, ntp) for d in range(ntp)]
    fetch = pltpu.make_async_copy(w_hbm, w_ref, wsem)
    fetch.start()
    local = [
        pltpu.make_async_copy(
            g_ref.at[:, pl.ds(f * depth, depth)], held.at[z, x, f], csem.at[f]
        )
        for f in range(halves)
    ]
    for f in range(halves):
        local[f].start()

    up, down = z < nz - 1, z > 0
    barrier = pltpu.get_barrier_semaphore()
    for d in range(1, nx):
        pl.semaphore_signal(barrier, inc=1, device_id=(z * nx + x_at[d], tp), device_id_type=MESH)
    for d in range(1, ntp):
        pl.semaphore_signal(barrier, inc=1, device_id=(kv, t_at[d]), device_id_type=MESH)
    for d in range(1, nz):
        pl.semaphore_signal(
            barrier, inc=1, device_id=(lax.rem(z + d, nz) * nx + x, tp), device_id_type=MESH
        )
    pl.semaphore_wait(barrier, nx - 1 + ntp - 1 + nz - 1)

    def along_z(origin, f, step):
        return remote(held.at[origin, x, f], held.at[origin, x, f], zss.at[origin, f, (step + 1) // 2],
                      zrs.at[origin, f], (kv + step * nx, tp))

    def along_x(origin, f, d):
        return remote(held.at[origin, x, f], held.at[origin, x, f], xss.at[origin, f, d],
                      xrs.at[origin, f, d], (z * nx + x_at[d], tp))

    def landed_x(origin, f, d):
        source = lax.rem(x + nx - d, nx)
        return remote(held.at[origin, x, f], held.at[origin, source, f], xss.at[origin, f, d],
                      xrs.at[origin, f, d], (z * nx + x_at[d], tp))

    for f in range(halves):
        local[f].wait()
        for side, step in ((up, 1), (down, -1)):
            @pl.when(side)
            def _():
                along_z(z, f, step).start()
        for d in range(1, nx):
            along_x(z, f, d).start()

    def multiply(origin):
        product = jnp.zeros((nx * rows, w_ref.shape[1]), jnp.float32)
        for f in range(halves):
            for d in range(1, nx):
                landed_x(origin, f, d).wait_recv()
            product = product + jnp.dot(
                held[origin, :, f].reshape(nx * rows, depth), w_ref[f * depth:(f + 1) * depth],
                preferred_element_type=jnp.float32,
            )
        for j in range(pieces):
            target = origin * pieces + j
            parts[target] = product[j * per:(j + 1) * per].astype(jnp.bfloat16)

            @pl.when(target != tp)
            def _():
                remote(parts.at[target], got.at[tp], tss.at[target], trs.at[tp],
                       (kv, target)).start()

    def relay(k):
        for f in range(halves):
            for step in (1, -1):
                origin = z - step * k

                @pl.when((origin >= 0) & (origin < nz))
                def _():
                    along_z(origin, f, step).wait_recv()
                    follow = up if step == 1 else down

                    @pl.when(follow)
                    def _():
                        along_z(origin, f, step).start()

                    for d in range(1, nx):
                        along_x(origin, f, d).start()

    for k in range(1, nz):
        relay(k)
        if k == 1:
            fetch.wait()
            multiply(z)
        for step in (1, -1):
            near = z - step * (k - 1)
            if k > 1:
                @pl.when((near >= 0) & (near < nz))
                def _():
                    multiply(near)
    if nz == 1:
        fetch.wait()
        multiply(z)
    else:
        for step in (1, -1):
            last = z - step * (nz - 1)

            @pl.when((last >= 0) & (last < nz))
            def _():
                multiply(last)

    summed = parts[tp].astype(jnp.float32)
    for d in range(1, ntp):
        source = t_at[d]
        remote(parts.at[source], got.at[source], tss.at[source], trs.at[source],
               (kv, source)).wait()
        summed = summed + got[source].astype(jnp.float32)
    out_ref[...] = summed.astype(out_ref.dtype)
    for f in range(halves):
        for origin in range(nz):
            for d in range(1, nx):
                along_x(origin, f, d).wait_send()

            @pl.when(up & (origin <= z))
            def _():
                along_z(origin, f, 1).wait_send()

            @pl.when(down & (origin >= z))
            def _():
                along_z(origin, f, -1).wait_send()


def output(nx, nz, ntp, gated, w_out):
    rows, depth = gated.shape
    columns = w_out.shape[1]
    halves = 2
    per = rows * nx * nz // ntp
    bf, dma = jnp.bfloat16, pltpu.SemaphoreType.DMA
    vmem = pl.BlockSpec(memory_space=pltpu.VMEM)
    return pl.pallas_call(
        functools.partial(output_kernel, nx, nz, ntp),
        out_shape=jax.ShapeDtypeStruct((per, columns), bf),
        in_specs=[vmem, pl.BlockSpec(memory_space=pl.ANY)],
        out_specs=vmem,
        scratch_shapes=[
            pltpu.VMEM((nz, nx, halves, rows, depth // halves), bf),
            pltpu.VMEM((ntp, per, columns), bf),
            pltpu.VMEM((ntp, per, columns), bf),
            pltpu.VMEM(w_out.shape, bf),
            dma((nz, halves, 2)), dma((nz, halves)), dma((nz, halves, nx)), dma((nz, halves, nx)),
            dma((ntp,)), dma((ntp,)), dma((halves,)), dma(()),
        ],
        compiler_params=pltpu.CompilerParams(
            collective_id=1, has_side_effects=True, vmem_limit_bytes=VMEM_LIMIT
        ),
    )(gated, w_out)


def per_device(
    nkv, ntp, hidden, norm_gain, w_query, w_key, w_value, w_gate, w_write, w_decay, w_out,
    decay_rate, head_gain, carried_state, last_keys, last_values, last_writes, last_decays,
    accepted,
):
    nz = 4 if nkv % 4 == 0 else 1
    nx = nkv // nz
    local_width = hidden.shape[1]
    heads = carried_state.shape[1]
    gain = lax.dynamic_slice_in_dim(norm_gain, lax.axis_index("kv") * local_width, local_width)
    w_small = jnp.concatenate(
        [w_write, w_decay, jnp.zeros((local_width, LANES - 2 * heads), w_write.dtype)], 1
    )
    plan, (projected, small) = project(
        nx, nz, hidden, gain[None, :], w_small, (w_query, w_key, w_value, w_gate),
        2 * heads, local_width * nkv,
    )
    gated, committed = core(
        plan, projected, small, last_keys, last_values, last_writes, last_decays,
        accepted[:, None], decay_rate[None, :], head_gain[None, :], carried_state,
    )
    return (output(nx, nz, ntp, gated, w_out), committed)


def solution(mesh):
    return jax.shard_map(
        functools.partial(per_device, mesh.shape["kv"], mesh.shape["tp"]),
        mesh=mesh,
        in_specs=(
            P(None, "kv"),
            P(),
            P("kv", "tp"),
            P("kv", "tp"),
            P("kv", "tp"),
            P("kv", "tp"),
            P("kv", "tp"),
            P("kv", "tp"),
            P("tp", "kv"),
            P("tp"),
            P(),
            P("kv", "tp", None, None),
            P("kv", None, "tp"),
            P("kv", None, "tp"),
            P("kv", None, "tp"),
            P("kv", None, "tp"),
            P("kv"),
        ),
        out_specs=(P("tp", "kv"), P("kv", "tp", None, None)),
        check_vma=False,
    )
```

```python
import functools
import jax
import jax.numpy as jnp
from jax import lax
from jax.experimental import pallas as pl
from jax.experimental.pallas import tpu as pltpu
from jax.sharding import PartitionSpec as P

norm_eps = 1e-06
LANES = 128
MESH = pl.DeviceIdType.MESH
VMEM_LIMIT = 60 * 1024 * 1024


def remote(src, dst, send, recv, device):
    return pltpu.make_async_remote_copy(
        src_ref=src, dst_ref=dst, send_sem=send, recv_sem=recv,
        device_id=device, device_id_type=MESH,
    )


def project_kernel(
    nx, nz, plan, width, sq_col, h_ref, n_ref, ws_ref, wq, wk, wv, wg, out_ref, small_out,
    s_ref, small_ref, wbuf, own, xs, xr, zs, zr, sm_xr, sm_zs, sm_zr,
    wsem, xss, xrs, zss, zrs, sxs, sxr, szs, szr,
):
    kv, tp = lax.axis_index("kv"), lax.axis_index("tp")
    x, z = lax.rem(kv, nx), lax.div(kv, nx)
    weights = (wq, wk, wv, wg)
    nc = len(plan)
    rows, cw = out_ref.shape[1], out_ref.shape[2]
    x_at = [lax.rem(x + d, nx) for d in range(nx)]
    z_at = [lax.rem(z + d, nz) for d in range(nz)]

    def fetch(c):
        which, off = plan[c]
        return pltpu.make_async_copy(
            weights[which].at[:, pl.ds(off, cw)], wbuf.at[c], wsem.at[c]
        )

    for c in range(nc):
        fetch(c).start()
    barrier = pltpu.get_barrier_semaphore()
    for d in range(1, nx):
        pl.semaphore_signal(barrier, inc=1, device_id=(z * nx + x_at[d], tp), device_id_type=MESH)
    for d in range(1, nz):
        pl.semaphore_signal(barrier, inc=1, device_id=(z_at[d] * nx + x, tp), device_id_type=MESH)
    gain = n_ref[...].astype(jnp.float32)
    lane = lax.broadcasted_iota(jnp.int32, (rows, LANES), 1)
    for i in range(nx):
        for j in range(nz):
            wide = h_ref[(j * nx + i) * rows:(j * nx + i + 1) * rows].astype(jnp.float32)
            scaled = (wide * gain).astype(jnp.bfloat16)
            s_ref[i, j * rows:(j + 1) * rows] = scaled
            part = jnp.dot(scaled, ws_ref[...], preferred_element_type=jnp.float32)
            square = jnp.sum(wide * wide, -1, keepdims=True)
            small_ref[i, j] = jnp.where(lane == sq_col, square, part).astype(jnp.bfloat16)
    pl.semaphore_wait(barrier, nx - 1 + nz - 1)

    def small_x(d):
        return remote(small_ref.at[x_at[d]], sm_xr.at[d - 1], sxs.at[d - 1], sxr.at[d - 1],
                      (z * nx + x_at[d], tp))

    def small_z(d):
        return remote(sm_zs.at[z_at[d]], sm_zr.at[d - 1], szs.at[d - 1], szr.at[d - 1],
                      (z_at[d] * nx + x, tp))

    def big_x(c, d):
        return remote(xs.at[c, d - 1], xr.at[c, d - 1], xss.at[c, d - 1], xrs.at[c, d - 1],
                      (z * nx + x_at[d], tp))

    def big_z(c, d):
        return remote(zs.at[c, z_at[d]], zr.at[c, d - 1], zss.at[c, d - 1], zrs.at[c, d - 1],
                      (z_at[d] * nx + x, tp))

    z_order = sorted(range(1, nz), key=lambda d: -min(d, nz - d))
    for d in range(1, nx):
        small_x(d).start()

    def multiply(c, carry):
        pltpu.make_async_copy(wbuf.at[c], wbuf.at[c], wsem.at[c]).wait()
        for d in range(1, nx):
            part = jnp.dot(s_ref[x_at[d]], wbuf[c], preferred_element_type=jnp.float32)
            xs[c, d - 1] = part.astype(jnp.bfloat16).reshape(nz, rows, cw)
            big_x(c, d).start()
        own[c] = jnp.dot(
            s_ref[x], wbuf[c], preferred_element_type=jnp.float32
        ).reshape(nz, rows, cw)
        return carry

    lax.fori_loop(0, nc, multiply, 0)

    total = small_ref[x].astype(jnp.float32)
    for d in range(1, nx):
        small_x(d).wait()
        total = total + sm_xr[d - 1].astype(jnp.float32)
    sm_zs[...] = total.astype(jnp.bfloat16)
    for d in z_order:
        small_z(d).start()

    def middle(c, carry):
        summed = own[c]
        for d in range(1, nx):
            big_x(c, d).wait()
            summed = summed + xr[c, d - 1].astype(jnp.float32)
        own[c] = summed
        zs[c] = summed.astype(jnp.bfloat16)
        for d in z_order:
            big_z(c, d).start()
        return carry

    lax.fori_loop(0, nc, middle, 0)

    small = sm_zs[z].astype(jnp.float32)
    for d in range(1, nz):
        small_z(d).wait()
        small = small + sm_zr[d - 1].astype(jnp.float32)
    inverse = lax.rsqrt(small[:, sq_col:sq_col + 1] / width + norm_eps)
    small_out[...] = small * inverse

    def finish(c, carry):
        summed = own[c, z]
        for d in range(1, nz):
            big_z(c, d).wait()
            summed = summed + zr[c, d - 1].astype(jnp.float32)
        out_ref[c] = summed * inverse
        return carry

    lax.fori_loop(0, nc, finish, 0)


def project(nx, nz, hidden, gain, w_small, weights, sq_col, width):
    depth = hidden.shape[1]
    rows = hidden.shape[0] // (nx * nz)
    cw = min(512, weights[0].shape[1])
    plan = [(i, off) for i, w in enumerate(weights) for off in range(0, w.shape[1], cw)]
    nc = len(plan)
    bf, f32, dma = jnp.bfloat16, jnp.float32, pltpu.SemaphoreType.DMA
    px, pz = max(nx - 1, 1), max(nz - 1, 1)
    vmem = pl.BlockSpec(memory_space=pltpu.VMEM)
    hbm = pl.BlockSpec(memory_space=pl.ANY)
    return plan, pl.pallas_call(
        functools.partial(project_kernel, nx, nz, plan, width, sq_col),
        out_shape=(
            jax.ShapeDtypeStruct((nc, rows, cw), f32),
            jax.ShapeDtypeStruct((rows, LANES), f32),
        ),
        in_specs=[vmem, vmem, vmem, hbm, hbm, hbm, hbm],
        out_specs=(vmem, vmem),
        scratch_shapes=[
            pltpu.VMEM((nx, nz * rows, depth), bf),
            pltpu.VMEM((nx, nz, rows, LANES), bf),
            pltpu.VMEM((nc, depth, cw), bf),
            pltpu.VMEM((nc, nz, rows, cw), f32),
            pltpu.VMEM((nc, px, nz, rows, cw), bf),
            pltpu.VMEM((nc, px, nz, rows, cw), bf),
            pltpu.VMEM((nc, nz, rows, cw), bf),
            pltpu.VMEM((nc, pz, rows, cw), bf),
            pltpu.VMEM((px, nz, rows, LANES), bf),
            pltpu.VMEM((nz, rows, LANES), bf),
            pltpu.VMEM((pz, rows, LANES), bf),
            dma((nc,)),
            dma((nc, px)), dma((nc, px)), dma((nc, pz)), dma((nc, pz)),
            dma((px,)), dma((px,)), dma((pz,)), dma((pz,)),
        ],
        compiler_params=pltpu.CompilerParams(
            collective_id=0, has_side_effects=True, vmem_limit_bytes=VMEM_LIMIT
        ),
    )(hidden, gain, w_small, *weights)


def silu(v):
    return v * jax.nn.sigmoid(v)


def unit(v):
    return v * lax.rsqrt(jnp.sum(v * v, -1, keepdims=True) + norm_eps)


def solve(keys, values, write, decay):
    steps = len(keys)
    running = [decay[0]]
    for t in range(1, steps):
        running.append(running[-1] + decay[t])
    strong = [keys[t] * write[t] for t in range(steps)]
    u_val, u_key = [], []
    for t in range(steps):
        cur_v = values[t] * write[t]
        cur_k = strong[t] * jnp.exp(running[t])
        for s in range(t):
            low = jnp.sum(strong[t] * keys[s], -1, keepdims=True)
            low = low * jnp.exp(running[t] - running[s])
            cur_v = cur_v - low * u_val[s]
            cur_k = cur_k - low * u_key[s]
        u_val.append(cur_v)
        u_key.append(cur_k)
    return running, u_val, u_key


def core_kernel(
    heads, q_ref, k_ref, v_ref, g_ref, small_ref, lk_ref, lv_ref, lsmall_ref, rate_ref,
    gain_ref, state_ref, gated_ref, com_ref, left, prod, kd, fr, dec, old_k, old_v, wide_v, gout,
):
    h = pl.program_id(0)
    seqs = state_ref.shape[0]
    steps = q_ref.shape[1] // seqs
    dk, dv = q_ref.shape[2], v_ref.shape[2]
    pad = kd.shape[1]
    bf, f32 = jnp.bfloat16, jnp.float32

    def at_t(ref, t):
        return ref[pl.ds(t, seqs, stride=steps), :]

    tiles = dv // LANES

    def value_at(ref, t):
        return jnp.concatenate([at_t(ref.at[j], t) for j in range(tiles)], -1)

    def cut(j):
        return slice(j * LANES, (j + 1) * LANES)

    lane = lax.broadcasted_iota(jnp.int32, (seqs, LANES), 1)

    few = lax.broadcasted_iota(jnp.int32, (seqs, heads), 1)

    def column(mat, col):
        index = lane if mat.shape[1] == LANES else few
        return jnp.sum(jnp.where(index == col, mat, 0.0), -1, keepdims=True)

    rate = column(jnp.broadcast_to(rate_ref[...], (seqs, heads)), h)
    every = range(steps)

    old_k[...] = lk_ref[...].astype(f32)
    old_v[...] = lv_ref[...].astype(f32)
    old = [at_t(lsmall_ref, t) for t in every]
    taken = [column(m, 2 * heads) for m in old]
    write = [jax.nn.sigmoid(column(old[t], h)) * taken[t] for t in every]
    decay = [-rate * jax.nn.softplus(column(old[t], heads + h)) * taken[t] for t in every]
    keys = [unit(old_k[:, t, :]) for t in every]
    running, old_val, u_key = solve(keys, [old_v[:, t, :] for t in every], write, decay)
    faded = [keys[t] * jnp.exp(running[-1] - running[t]) for t in every]
    kept = jnp.exp(running[-1])
    for t in every:
        left[:, t, :] = u_key[t]
        kd[:, t, :] = faded[t]
    dec[...] = jnp.broadcast_to(kept, (seqs, dv))
    for t in range(steps, pad):
        kd[:, t, :] = jnp.zeros((seqs, dk), f32)
        fr[:, t, :] = jnp.zeros((seqs, dv), f32)
    for t in range(3 * steps, left.shape[1]):
        left[:, t, :] = jnp.zeros((seqs, dk), f32)

    small = [at_t(small_ref, t) for t in every]
    write = [jax.nn.sigmoid(column(small[t], h)) for t in every]
    decay = [-rate * jax.nn.softplus(column(small[t], heads + h)) for t in every]
    queries = [unit(silu(at_t(q_ref.at[0], t))) * dk ** (-0.5) for t in every]
    for j in range(tiles):
        wide_v[j] = silu(v_ref[0, :, cut(j)])
    keys = [unit(silu(at_t(k_ref.at[0], t))) for t in every]
    running, u_val, u_key = solve(keys, [value_at(wide_v, t) for t in every], write, decay)
    rotated = [queries[t] * jnp.exp(running[t]) for t in every]
    for t in every:
        left[:, steps + t, :] = u_key[t]
        left[:, 2 * steps + t, :] = rotated[t]
    for b in range(seqs):
        prod[b] = jnp.dot(
            left[b].astype(bf), state_ref[b, 0].astype(bf), preferred_element_type=f32
        )
    old_fresh = [old_val[t] - prod[:, t, :] for t in every]
    for t in every:
        fr[:, t, :] = old_fresh[t]
    for b in range(seqs):
        added = lax.dot_general(
            kd[b].astype(bf), fr[b].astype(bf), (((0,), (0,)), ((), ())),
            preferred_element_type=f32,
        )
        com_ref[b, 0] = state_ref[b, 0] * dec[b:b + 1, :] + added

    def through(rows, at):
        total = kept * prod[:, at, :]
        for s in every:
            total = total + jnp.sum(rows * faded[s], -1, keepdims=True) * old_fresh[s]
        return total

    gain = gain_ref[...]
    fresh = [u_val[t] - through(u_key[t], steps + t) for t in every]
    for t in every:
        result = through(rotated[t], 2 * steps + t)
        for s in range(t + 1):
            score = jnp.sum(queries[t] * keys[s], -1, keepdims=True)
            score = score * jnp.exp(running[t] - running[s])
            result = result + score * fresh[s]
        scale = lax.rsqrt(jnp.mean(result * result, -1, keepdims=True) + norm_eps)
        normed = result * scale * gain
        for j in range(tiles):
            gout[j, pl.ds(t, seqs, stride=steps), :] = normed[:, cut(j)]
    for j in range(tiles):
        gated_ref[:, cut(j)] = (gout[j] * silu(g_ref[0, :, cut(j)])).astype(bf)


def core(plan, projected, small, last_keys, last_values, last_small, rates, head_gain, state):
    seqs, heads, dk, dv = state.shape
    steps = last_keys.shape[1]
    rows = seqs * steps
    cw = projected.shape[2]
    kpc, vpc = cw // dk, cw // dv
    first = [next(c for c, (w, _) in enumerate(plan) if w == i) for i in range(4)]
    pad = 2 * steps
    f32 = jnp.float32

    def key_block(base):
        return pl.BlockSpec((1, rows, dk), lambda h: (base + h // kpc, 0, h % kpc))

    def val_block(base):
        return pl.BlockSpec((1, rows, dv), lambda h: (base + h // vpc, 0, h % vpc))

    def whole(shape):
        return pl.BlockSpec(shape, lambda h: (0,) * len(shape))

    state_block = pl.BlockSpec((seqs, 1, dk, dv), lambda h: (0, h, 0, 0))
    return pl.pallas_call(
        functools.partial(core_kernel, heads),
        grid=(heads,),
        out_shape=(
            jax.ShapeDtypeStruct((rows, heads * dv), jnp.bfloat16),
            jax.ShapeDtypeStruct(state.shape, f32),
        ),
        in_specs=[
            key_block(first[0]), key_block(first[1]), val_block(first[2]), val_block(first[3]),
            whole((rows, LANES)),
            pl.BlockSpec((seqs, steps, dk), lambda h: (0, 0, h)),
            pl.BlockSpec((seqs, steps, dv), lambda h: (0, 0, h)),
            whole((rows, LANES)), whole((1, heads)), whole((1, dv)), state_block,
        ],
        out_specs=(pl.BlockSpec((rows, dv), lambda h: (0, h)), state_block),
        scratch_shapes=[
            pltpu.VMEM((seqs, 2 * pad, dk), f32),
            pltpu.VMEM((seqs, 2 * pad, dv), f32),
            pltpu.VMEM((seqs, pad, dk), f32),
            pltpu.VMEM((seqs, pad, dv), f32),
            pltpu.VMEM((seqs, dv), f32),
            pltpu.VMEM((seqs, steps, dk), f32),
            pltpu.VMEM((seqs, steps, dv), f32),
            pltpu.VMEM((dv // LANES, rows, LANES), f32),
            pltpu.VMEM((dv // LANES, rows, LANES), f32),
        ],
        compiler_params=pltpu.CompilerParams(vmem_limit_bytes=VMEM_LIMIT),
    )(
        projected, projected, projected, projected, small,
        last_keys, last_values, last_small, rates, head_gain, state,
    )


def output_kernel(
    nx, nz, ntp, g_ref, w_hbm, out_ref, held, parts, got, w_ref,
    zss, zrs, xss, xrs, tss, trs, csem, wsem,
):
    kv, tp = lax.axis_index("kv"), lax.axis_index("tp")
    x, z = lax.rem(kv, nx), lax.div(kv, nx)
    halves, rows, depth = held.shape[2:]
    per = out_ref.shape[0]
    pieces = nx * rows // per
    x_at = [lax.rem(x + d, nx) for d in range(nx)]
    t_at = [lax.rem(tp + d, ntp) for d in range(ntp)]
    fetch = pltpu.make_async_copy(w_hbm, w_ref, wsem)
    fetch.start()
    local = [
        pltpu.make_async_copy(
            g_ref.at[:, pl.ds(f * depth, depth)], held.at[z, x, f], csem.at[f]
        )
        for f in range(halves)
    ]
    for f in range(halves):
        local[f].start()

    up, down = z < nz - 1, z > 0
    barrier = pltpu.get_barrier_semaphore()
    for d in range(1, nx):
        pl.semaphore_signal(barrier, inc=1, device_id=(z * nx + x_at[d], tp), device_id_type=MESH)
    for d in range(1, ntp):
        pl.semaphore_signal(barrier, inc=1, device_id=(kv, t_at[d]), device_id_type=MESH)
    for d in range(1, nz):
        pl.semaphore_signal(
            barrier, inc=1, device_id=(lax.rem(z + d, nz) * nx + x, tp), device_id_type=MESH
        )
    pl.semaphore_wait(barrier, nx - 1 + ntp - 1 + nz - 1)

    def along_z(origin, f, step):
        return remote(held.at[origin, x, f], held.at[origin, x, f], zss.at[origin, f, (step + 1) // 2],
                      zrs.at[origin, f], (kv + step * nx, tp))

    def along_x(origin, f, d):
        return remote(held.at[origin, x, f], held.at[origin, x, f], xss.at[origin, f, d],
                      xrs.at[origin, f, d], (z * nx + x_at[d], tp))

    def landed_x(origin, f, d):
        source = lax.rem(x + nx - d, nx)
        return remote(held.at[origin, x, f], held.at[origin, source, f], xss.at[origin, f, d],
                      xrs.at[origin, f, d], (z * nx + x_at[d], tp))

    for f in range(halves):
        local[f].wait()
        for side, step in ((up, 1), (down, -1)):
            @pl.when(side)
            def _():
                along_z(z, f, step).start()
        for d in range(1, nx):
            along_x(z, f, d).start()

    def multiply(origin):
        product = jnp.zeros((nx * rows, w_ref.shape[1]), jnp.float32)
        for f in range(halves):
            for d in range(1, nx):
                landed_x(origin, f, d).wait_recv()
            product = product + jnp.dot(
                held[origin, :, f].reshape(nx * rows, depth), w_ref[f * depth:(f + 1) * depth],
                preferred_element_type=jnp.float32,
            )
        for j in range(pieces):
            target = origin * pieces + j
            parts[target] = product[j * per:(j + 1) * per].astype(jnp.bfloat16)

            @pl.when(target != tp)
            def _():
                remote(parts.at[target], got.at[tp], tss.at[target], trs.at[tp],
                       (kv, target)).start()

    def relay(k):
        for f in range(halves):
            for step in (1, -1):
                origin = z - step * k

                @pl.when((origin >= 0) & (origin < nz))
                def _():
                    along_z(origin, f, step).wait_recv()
                    follow = up if step == 1 else down

                    @pl.when(follow)
                    def _():
                        along_z(origin, f, step).start()

                    for d in range(1, nx):
                        along_x(origin, f, d).start()

    for k in range(1, nz):
        relay(k)
        if k == 1:
            fetch.wait()
            multiply(z)
        for step in (1, -1):
            near = z - step * (k - 1)
            if k > 1:
                @pl.when((near >= 0) & (near < nz))
                def _():
                    multiply(near)
    if nz == 1:
        fetch.wait()
        multiply(z)
    else:
        for step in (1, -1):
            last = z - step * (nz - 1)

            @pl.when((last >= 0) & (last < nz))
            def _():
                multiply(last)

    summed = parts[tp].astype(jnp.float32)
    for d in range(1, ntp):
        source = t_at[d]
        remote(parts.at[source], got.at[source], tss.at[source], trs.at[source],
               (kv, source)).wait()
        summed = summed + got[source].astype(jnp.float32)
    out_ref[...] = summed.astype(out_ref.dtype)
    for f in range(halves):
        for origin in range(nz):
            for d in range(1, nx):
                along_x(origin, f, d).wait_send()

            @pl.when(up & (origin <= z))
            def _():
                along_z(origin, f, 1).wait_send()

            @pl.when(down & (origin >= z))
            def _():
                along_z(origin, f, -1).wait_send()


def output(nx, nz, ntp, gated, w_out):
    rows, depth = gated.shape
    columns = w_out.shape[1]
    halves = 2
    per = rows * nx * nz // ntp
    bf, dma = jnp.bfloat16, pltpu.SemaphoreType.DMA
    vmem = pl.BlockSpec(memory_space=pltpu.VMEM)
    return pl.pallas_call(
        functools.partial(output_kernel, nx, nz, ntp),
        out_shape=jax.ShapeDtypeStruct((per, columns), bf),
        in_specs=[vmem, pl.BlockSpec(memory_space=pl.ANY)],
        out_specs=vmem,
        scratch_shapes=[
            pltpu.VMEM((nz, nx, halves, rows, depth // halves), bf),
            pltpu.VMEM((ntp, per, columns), bf),
            pltpu.VMEM((ntp, per, columns), bf),
            pltpu.VMEM(w_out.shape, bf),
            dma((nz, halves, 2)), dma((nz, halves)), dma((nz, halves, nx)), dma((nz, halves, nx)),
            dma((ntp,)), dma((ntp,)), dma((halves,)), dma(()),
        ],
        compiler_params=pltpu.CompilerParams(
            collective_id=1, has_side_effects=True, vmem_limit_bytes=VMEM_LIMIT
        ),
    )(gated, w_out)


def per_device(
    nkv, ntp, hidden, norm_gain, w_query, w_key, w_value, w_gate, w_write, w_decay, w_out,
    decay_rate, head_gain, carried_state, last_keys, last_values, last_writes, last_decays,
    accepted,
):
    nz = 4 if nkv % 4 == 0 else 1
    nx = nkv // nz
    local_width = hidden.shape[1]
    heads = carried_state.shape[1]
    gain = lax.dynamic_slice_in_dim(norm_gain, lax.axis_index("kv") * local_width, local_width)
    w_small = jnp.concatenate(
        [w_write, w_decay, jnp.zeros((local_width, LANES - 2 * heads), w_write.dtype)], 1
    )
    plan, (projected, small) = project(
        nx, nz, hidden, gain[None, :], w_small, (w_query, w_key, w_value, w_gate),
        2 * heads, local_width * nkv,
    )
    seqs, steps = last_keys.shape[:2]
    rows = seqs * steps
    taken = (jnp.arange(steps, dtype=jnp.int32)[None, :] < accepted[:, None]).astype(jnp.float32)
    last_small = jnp.concatenate(
        [last_writes.reshape(rows, heads), last_decays.reshape(rows, heads),
         taken.reshape(rows, 1), jnp.zeros((rows, LANES - 2 * heads - 1), jnp.float32)], 1
    )
    gated, committed = core(
        plan, projected, small, last_keys, last_values, last_small, decay_rate[None, :],
        head_gain[None, :], carried_state,
    )
    return (output(nx, nz, ntp, gated, w_out), committed)


def solution(mesh):
    return jax.shard_map(
        functools.partial(per_device, mesh.shape["kv"], mesh.shape["tp"]),
        mesh=mesh,
        in_specs=(
            P(None, "kv"),
            P(),
            P("kv", "tp"),
            P("kv", "tp"),
            P("kv", "tp"),
            P("kv", "tp"),
            P("kv", "tp"),
            P("kv", "tp"),
            P("tp", "kv"),
            P("tp"),
            P(),
            P("kv", "tp", None, None),
            P("kv", None, "tp"),
            P("kv", None, "tp"),
            P("kv", None, "tp"),
            P("kv", None, "tp"),
            P("kv"),
        ),
        out_specs=(P("tp", "kv"), P("kv", "tp", None, None)),
        check_vma=False,
    )
```
